32 devices in a mesh: ep: 8 (over z, x), tp: 4 (over y, core).
Axes of the slice: x: 2, y: 2, z: 4, core: 2. Of those that a mesh axis runs over, the one named last changes fastest.
Arguments:
- tokens: bfloat16 [6144, 2048], P(('ep', 'tp')), may hold values from -6 to 6
- routes: int32 [6144, 2], P(('ep', 'tp')), may hold values from 0 to 7, all different within a row; in each aligned block of 192 rows (0 to 191, 192 to 383, ...) at most 64 rows name the same one
- gates: float32 [6144, 2], P(('ep', 'tp')), may hold values from 0.3 to 2.2
- pre_gain: float32 [2048], replicated, may hold values from 0.1 to 1.9
- w_gate: bfloat16 [8, 2048, 512], P('ep'), may hold values from -0.125 to 0.125
- w_up: bfloat16 [8, 2048, 512], P('ep'), may hold values from -0.125 to 0.125
- w_down: bfloat16 [8, 512, 2048], P('ep'), may hold values from -0.25 to 0.25
- sh_gate: bfloat16 [2048, 512], P('tp'), may hold values from -0.125 to 0.125
- sh_up: bfloat16 [2048, 512], P('tp'), may hold values from -0.125 to 0.125
- sh_down: bfloat16 [512, 2048], P(None, 'tp'), may hold values from -0.25 to 0.25
- post_gain: float32 [2048], replicated, may hold values from 0.1 to 1.9
Outputs:
- mixed: bfloat16 [6144, 2048], P('ep', 'tp')
The draws below stay inside these ranges and needn't reach their ends.
Inputs may be any that keep to these rules, and one draw needn't show every extreme that they name: `routes`: each token names 2 different experts; among the rows of one device no expert is named more than 64 times, a bound that some block reaches.
All inputs are finite; a program needn't handle non-finite values.
Results may differ from the reference program's by a relative error of at most 0.0075.
Values may be sent and summed in bfloat16 or wider, within the bound.
No kernel may reach another device: no remote copies, remote signals or barrier semaphores. Data moves between devices by JAX's collectives and lax.ppermute only.
A program may use at most 64 MiB of HBM per device.

```python
import math
import jax
import jax.numpy as jnp
import numpy as np
from jax import lax

D = 2048
FF = 512
SH = 512
TOPK = 2
TOK_DEV = 192
EXPERTS = 8
CAP = 64
TOKENS = 6144
N_EP = 8
N_TP = 4


def levels(key, shape, shards, smallest, largest):
    def one(axis_at, parts):
        draws = jax.random.uniform(jax.random.fold_in(jax.random.fold_in(key, 6), axis_at), (parts,), jnp.float32, smallest / len(shards), largest / len(shards))
        return jnp.repeat(jnp.exp(draws), shape[axis_at] // parts).reshape((-1,) + (1,) * (len(shape) - axis_at - 1))

    factor_of = one(*shards[0])
    for cut in shards[1:]:
        factor_of = factor_of * one(*cut)
    return factor_of


def assign_block(stream_key, own, number, rows, amount, top, limit, skew):
    ranking = jax.random.permutation(stream_key, amount)
    crowded, ordinary = portions_of(amount, rows * top, limit, skew, True), portions_of(amount, rows * top, limit, skew, False)
    places = jnp.arange(amount)

    def named(lengths, turn):
        used = int((lengths > 0).sum())
        fixed = max(1, used // 4)
        passed = fixed + (places - fixed + turn * (used - fixed)) % max(1, amount - fixed)
        return jnp.zeros((amount,), jnp.int32).at[ranking[jnp.where(places < fixed, places, passed)]].set(jnp.asarray(lengths, jnp.int32))

    lengths = jnp.where(number % 4 == 0, named(crowded, number // 4), named(ordinary, number - number // 4 - 1))
    mixed = jax.random.permutation(jax.random.fold_in(own, 3), amount)
    source_of, taker = mixed[0:amount // 2 * 2:2], mixed[1:amount // 2 * 2:2]
    margin = jnp.minimum(lengths[source_of] - 1, limit - lengths[taker]) // 2
    margin = jnp.where((source_of == ranking[0]) | (taker == ranking[0]) | (lengths[taker] == 0), 0, jnp.maximum(margin, 0))
    passed = jax.random.randint(jax.random.fold_in(own, 4), (amount // 2,), 0, 1 << 20) % (margin + 1)
    lengths = lengths.at[source_of].add(-passed).at[taker].add(passed)
    members = jnp.searchsorted(jnp.cumsum(lengths), jnp.arange(rows * top), side="right").astype(jnp.int32)
    grid = members.reshape(top, rows).T
    grid = grid[jax.random.permutation(jax.random.fold_in(own, 1), rows)]
    turn = jax.random.randint(jax.random.fold_in(own, 2), (rows, 1), 0, top)
    return jnp.take_along_axis(grid, (jnp.arange(top)[None, :] + turn) % top, axis=1)


def portions_of(count, total, limit, slope, full):
    portions = [(1 << 20) // math.isqrt(standing ** slope) + 1 for standing in range(1, count + 1)]
    largest = limit if full else min(limit, max(-(-total // count), total * portions[0] // sum(portions)))
    least = 1 if total - largest >= count - 1 else 0
    counts, spare = [largest] + [least] * (count - 1), total - largest - least * (count - 1)
    while spare > 0:
        free = [i for i in range(1, count) if counts[i] < largest] or [i for i in range(1, count) if counts[i] < limit]
        mass, remaining = sum([portions[i] for i in free]), spare
        for i in free:
            addition = min(limit - counts[i], max(1, remaining * portions[i] // mass), spare)
            counts[i] = counts[i] + addition
            spare = spare - addition
    return np.array(counts)


def normal_values(key, shape, scale, reach, split=(), kind=jnp.bfloat16):
    drawn = jax.random.normal(key, shape, jnp.float32) * scale
    if len(split) > 0:
        drawn = levels(key, shape, split, -0.22, 0.18) * drawn
    return jnp.clip(drawn, min=-reach, max=reach).astype(kind)


def setup_inputs(seed: int = 0) -> dict:
    key_of = jax.random.split(jax.random.key(seed), 12)
    tokens = normal_values(key_of[0], (TOKENS, D), 1.0, 6.0, ((0, 32),))
    routes_keys = jax.random.split(jax.random.fold_in(key_of[1], 1), TOKENS // TOK_DEV)
    routes_turns = jax.random.permutation(jax.random.fold_in(key_of[1], 3), TOKENS // TOK_DEV)
    routes = jax.vmap(lambda own, number: assign_block(jax.random.fold_in(key_of[1], 2), own, number, TOK_DEV, EXPERTS, TOPK, CAP, 2))(routes_keys, routes_turns).reshape((TOKENS, TOPK))
    gates = jnp.clip(0.3 + 1.90000004 * jax.random.uniform(key_of[2], (TOKENS, TOPK), jnp.float32) ** levels(key_of[2], (TOKENS, TOPK), ((0, 32),), -0.2, 0.2), 0.3, 2.2)
    pre_gain = jnp.clip(1.0 + 0.18 * jax.random.normal(key_of[3], (D,), jnp.float32), 0.1, 1.9)
    w_gate = normal_values(key_of[4], (EXPERTS, D, FF), D ** -0.5, 0.125, ((0, 8),))
    w_up = normal_values(key_of[5], (EXPERTS, D, FF), D ** -0.5, 0.125, ((0, 8),))
    w_down = normal_values(key_of[6], (EXPERTS, FF, D), FF ** -0.5, 0.25, ((0, 8),))
    sh_gate = normal_values(key_of[7], (D, SH), D ** -0.5, 0.125, ((0, 4),))
    sh_up = normal_values(key_of[8], (D, SH), D ** -0.5, 0.125, ((0, 4),))
    sh_down = normal_values(key_of[9], (SH, D), SH ** -0.5, 0.25, ((1, 4),))
    post_gain = jnp.clip(1.0 + 0.18 * jax.random.normal(key_of[10], (D,), jnp.float32), 0.1, 1.9)
    return dict(tokens=tokens, routes=routes, gates=gates, pre_gain=pre_gain, w_gate=w_gate, w_up=w_up, w_down=w_down, sh_gate=sh_gate, sh_up=sh_up, sh_down=sh_down, post_gain=post_gain)


def rms_scale(values):
    return lax.rsqrt(lax.optimization_barrier(jnp.mean(values * values, axis=-1, keepdims=True)) + 1e-06)

def reference(tokens, routes, gates, pre_gain, w_gate, w_up, w_down, sh_gate, sh_up, sh_down, post_gain):
    devices_all = N_EP * N_TP
    per_device = TOK_DEV * TOPK
    inputs = tokens.astype(jnp.float32)
    normed = (inputs * rms_scale(inputs) * pre_gain.astype(jnp.float32)).astype(jnp.bfloat16)
    expert_ids = routes.reshape(devices_all, per_device).astype(jnp.int32)
    matches = (expert_ids[:, :, None] == jnp.arange(EXPERTS, dtype=jnp.int32)[None, None, :]).astype(jnp.int32)
    earlier = jnp.cumsum(matches, axis=1) - matches
    slot_index = lax.optimization_barrier(jnp.sum(earlier * matches, axis=2)).astype(jnp.int32)
    sources = jnp.broadcast_to(jnp.arange(devices_all, dtype=jnp.int32)[:, None], (devices_all, per_device))
    token_index = sources * TOK_DEV + jnp.arange(per_device, dtype=jnp.int32)[None, :] // TOPK
    table = jnp.full((EXPERTS, devices_all, CAP), TOKENS, jnp.int32).at[expert_ids, sources, slot_index].set(token_index)
    weight_table = jnp.zeros((EXPERTS, devices_all, CAP), jnp.float32).at[expert_ids, sources, slot_index].set(gates.reshape(devices_all, per_device).astype(jnp.float32))
    padded = jnp.concatenate([normed, jnp.zeros((1, D), jnp.bfloat16)], axis=0)

    def one_expert(summed, pack):
        rows_index, row_weight, gate_mat, up_mat, down_mat = pack
        picked = padded[rows_index]
        gate_part = jnp.dot(picked, gate_mat, preferred_element_type=jnp.float32)
        up_part = jnp.dot(picked, up_mat, preferred_element_type=jnp.float32)
        hidden = (jax.nn.silu(gate_part) * up_part).astype(jnp.bfloat16)
        result = jnp.dot(hidden, down_mat, preferred_element_type=jnp.float32).astype(jnp.bfloat16)
        summed = summed.at[rows_index].add(row_weight[:, None] * result.astype(jnp.float32))
        return (summed, None)
    summed, _ = lax.scan(one_expert, jnp.zeros((TOKENS + 1, D), jnp.float32), (table.reshape(EXPERTS, -1), weight_table.reshape(EXPERTS, -1), w_gate, w_up, w_down))
    routed = summed[:TOKENS].astype(jnp.bfloat16)
    gate_shared = jnp.dot(normed, sh_gate, preferred_element_type=jnp.float32)
    up_shared = jnp.dot(normed, sh_up, preferred_element_type=jnp.float32)
    shared_hidden = (jax.nn.silu(gate_shared) * up_shared).astype(jnp.bfloat16)
    shared = jnp.dot(shared_hidden, sh_down, preferred_element_type=jnp.float32).astype(jnp.bfloat16)
    combined = routed.astype(jnp.float32) + shared.astype(jnp.float32)
    return (combined * rms_scale(combined) * post_gain.astype(jnp.float32)).astype(jnp.bfloat16)
```

```python
import functools

import jax
import jax.numpy as jnp
from jax import lax
from jax.experimental import pallas as pl
from jax.experimental.pallas import tpu as pltpu
from jax.sharding import PartitionSpec as P

TOPK = 2
LANES = 128
EPS = 1e-06
F32, BF16 = jnp.float32, jnp.bfloat16
VMEM = pl.BlockSpec(memory_space=pltpu.VMEM)
SMEM = pl.BlockSpec(memory_space=pltpu.SMEM)


def dot(a, b):
    return jnp.dot(a, b, preferred_element_type=F32)


def silu(v):
    return v / (1.0 + jnp.exp(-v))


def cost(flops, moved):
    return pl.CostEstimate(flops=int(flops), bytes_accessed=int(moved), transcendentals=0)


def params():
    return pltpu.CompilerParams(vmem_limit_bytes=40 * 2**20)


def pre_kernel(capacity, me_ref, tok_ref, routes_ref, gates_ref, gain_ref, normed_ref, meta_ref, *bufs):
    rows, width = tok_ref.shape
    slots = capacity * len(bufs)
    x = tok_ref[...].astype(F32)
    scale = lax.rsqrt(jnp.mean(x * x, axis=1, keepdims=True) + EPS)
    normed_ref[...] = (x * scale * gain_ref[...]).astype(BF16)
    lane = lax.broadcasted_iota(jnp.int32, (rows, LANES), 1)
    rel = jnp.bitwise_xor(routes_ref[...], me_ref[0])
    first, second = rel[:, 0:1], rel[:, 1:2]
    hit0, hit1 = (first == lane).astype(F32), (second == lane).astype(F32)
    below = (
        lax.broadcasted_iota(jnp.int32, (rows, rows), 1)
        < lax.broadcasted_iota(jnp.int32, (rows, rows), 0)
    ).astype(F32).astype(BF16)
    before0 = dot(below, hit0.astype(BF16))
    before1 = dot(below, hit1.astype(BF16)) + jnp.sum(hit0, axis=0, keepdims=True)
    slot0 = jnp.sum(before0 * hit0, axis=1, keepdims=True).astype(jnp.int32)
    slot1 = jnp.sum(before1 * hit1, axis=1, keepdims=True).astype(jnp.int32)
    dest0, dest1 = first * capacity + slot0, second * capacity + slot1
    gates = gates_ref[...]
    meta = jnp.where(lane == 0, dest0.astype(F32), dest1.astype(F32))
    meta = jnp.where(lane == 2, gates[:, 0:1], jnp.where(lane == 3, gates[:, 1:2], meta))
    meta_ref[...] = meta
    place = lax.broadcasted_iota(jnp.int32, (rows, slots), 1)
    chosen = ((place == dest0) | (place == dest1)).astype(F32).astype(BF16)
    picked = lax.dot_general(
        chosen, normed_ref[...], (((0,), (0,)), ((), ())), preferred_element_type=F32
    ).astype(BF16)
    for j, buf in enumerate(bufs):
        buf[...] = picked[j * capacity : (j + 1) * capacity]


def gated_kernel(*refs):
    parts, (gate_ref, up_ref), out_ref = refs[:-3], refs[-3:-1], refs[-1]
    rows = jnp.concatenate([part[...] for part in parts], axis=0)
    gate, up = dot(rows, gate_ref[0]), dot(rows, up_ref[0])
    out_ref[...] = (silu(gate) * up).astype(BF16)


def shared_kernel(count, tp_ref, normed_ref, *refs):
    gates, ups, out_ref = refs[:count], refs[count : 2 * count], refs[-1]
    depth = gates[0].shape[0]
    gate = up = None
    for m in range(count):
        at = pl.multiple_of(jnp.bitwise_xor(tp_ref[0], m) * depth, depth)
        part = normed_ref[:, pl.ds(at, depth)]
        g, u = dot(part, gates[m][...]), dot(part, ups[m][...])
        gate, up = (g, u) if m == 0 else (gate + g, up + u)
    out_ref[...] = (silu(gate) * up).astype(BF16)


def shared_out_kernel(*refs):
    parts, down_ref, out_ref = refs[:-2], refs[-2], refs[-1]
    rows = parts[0].shape[0]
    for m, part in enumerate(parts):
        out_ref[m * rows : (m + 1) * rows] = dot(part[...], down_ref[...]).astype(BF16)


def combine_kernel(sources, experts, groups, capacity, *refs):
    hidden = refs[: sources * groups]
    downs = refs[sources * groups : sources * groups + experts]
    metas = refs[sources * groups + experts : sources * groups + experts + sources]
    shared_ref, comb_ref, squares_ref, result = refs[-4:]
    per_group = experts // groups
    for j in range(experts):
        low = (j % per_group) * capacity
        rows = jnp.concatenate(
            [hidden[m * groups + j // per_group][low : low + capacity] for m in range(sources)], axis=0
        )
        out = dot(rows, downs[j][...]).astype(BF16)
        for m in range(sources):
            result[m, j * capacity : (j + 1) * capacity] = out[m * capacity : (m + 1) * capacity]
    tokens = metas[0].shape[0]
    place = lax.broadcasted_iota(jnp.int32, (tokens, experts * capacity), 1)
    for m in range(sources):
        meta = metas[m][...]
        routed = None
        for k in range(TOPK):
            chosen = (place == meta[:, k : k + 1].astype(jnp.int32)).astype(F32).astype(BF16)
            term = dot(chosen, result[m]) * meta[:, TOPK + k : TOPK + k + 1]
            routed = term if k == 0 else routed + term
        here = slice(m * tokens, (m + 1) * tokens)
        combined = routed.astype(BF16).astype(F32) + shared_ref[here].astype(F32)
        comb_ref[here] = combined
        total = jnp.sum(combined * combined, axis=1, keepdims=True)
        squares_ref[m : m + 1] = jnp.broadcast_to(total, (tokens, LANES)).T[0:1]


def final_kernel(width, tp_ref, comb_ref, gain_ref, *refs):
    squares, out_ref = refs[:-1], refs[-1]
    count = len(squares)
    tokens = comb_ref.shape[0] // count
    gain = gain_ref[...]
    for m in range(count):
        total = squares[0][m : m + 1]
        for d in range(1, count):
            total = total + squares[d][m ^ d : (m ^ d) + 1]
        scale = lax.rsqrt(total / width + EPS)
        column = jnp.broadcast_to(scale, (LANES, tokens)).T[:, 0:1]
        at = pl.multiple_of(jnp.bitwise_xor(tp_ref[0], m) * tokens, 64)
        values = comb_ref[m * tokens : (m + 1) * tokens] * column * gain
        out_ref[pl.ds(at, tokens)] = values.astype(BF16)


def flip(value, axis, mask):
    size = lax.axis_size(axis)
    return lax.ppermute(value, axis, [(i, i ^ mask) for i in range(size)])


def gather_all(value, axis):
    size = lax.axis_size(axis)
    held = {0: value}
    mask = size // 2
    while mask:
        for j in list(held):
            held[j ^ mask] = flip(held[j], axis, mask)
        mask //= 2
    return [held[j] for j in range(size)]


def shape(dims, kind):
    return jax.ShapeDtypeStruct(dims, kind)


def folded(
    tokens, routes, gates, pre_gain, w_gate, w_up, w_down, sh_gate, sh_up, sh_down, post_gain, *, capacity
):
    rows, width = tokens.shape
    experts, sources = lax.axis_size("ep"), lax.axis_size("tp")
    inner, columns = w_down.shape[1], width // sources
    ep = lax.axis_index("ep").astype(jnp.int32).reshape(1)
    tp = lax.axis_index("tp").astype(jnp.int32).reshape(1)
    near = experts // 2

    normed, meta, *bufs = pl.pallas_call(
        functools.partial(pre_kernel, capacity),
        out_shape=[shape((rows, width), BF16), shape((rows, LANES), F32)]
        + [shape((capacity, width), BF16)] * experts,
        in_specs=[SMEM] + [VMEM] * 4,
        out_specs=[VMEM] * (2 + experts),
        compiler_params=params(),
        cost_estimate=cost(2 * rows * experts * capacity * width, 4 * rows * width),
        name="pre",
    )(ep, tokens, routes, gates, pre_gain.reshape(1, width))

    arrived = [bufs[0]] + [None] * (experts - 1)
    for j in list(range(near, experts)) + list(range(1, near)):
        arrived[j] = flip(bufs[j], "ep", j)

    downs = gather_all(lax.dynamic_slice_in_dim(w_down[0], tp[0] * columns, columns, axis=1), "ep")
    sh_gates, sh_ups = gather_all(sh_gate, "tp"), gather_all(sh_up, "tp")
    metas = gather_all(meta, "tp")

    shared_hidden = pl.pallas_call(
        functools.partial(shared_kernel, sources),
        out_shape=shape((rows, sh_down.shape[0]), BF16),
        in_specs=[SMEM] + [VMEM] * (1 + 2 * sources),
        out_specs=VMEM,
        compiler_params=params(),
        cost_estimate=cost(4 * rows * width * inner, 4 * width * inner),
        name="shared_hidden",
    )(tp, normed, *sh_gates, *sh_ups)
    shared = pl.pallas_call(
        shared_out_kernel,
        out_shape=shape((sources * rows, columns), BF16),
        in_specs=[VMEM] * (sources + 1),
        out_specs=VMEM,
        compiler_params=params(),
        cost_estimate=cost(2 * sources * rows * inner * columns, 2 * inner * columns),
        name="shared_out",
    )(*gather_all(shared_hidden, "tp"), sh_down)

    groups = 2
    hidden = []
    for g in range(groups):
        blocks = range(g * near, (g + 1) * near)
        out = pl.pallas_call(
            gated_kernel,
            out_shape=shape((near * capacity, inner), BF16),
            in_specs=[VMEM] * (near + 2),
            out_specs=VMEM,
            compiler_params=params(),
            cost_estimate=cost(4 * near * capacity * width * inner, 4 * width * inner),
            name="gated",
        )(*[arrived[j] for j in blocks], w_gate, w_up)
        back = []
        for b, j in enumerate(blocks):
            block = out[b * capacity : (b + 1) * capacity]
            back.append(block if j == 0 else flip(block, "ep", j))
        hidden.append(gather_all(jnp.concatenate(back, axis=0), "tp"))

    combined, squares = pl.pallas_call(
        functools.partial(combine_kernel, sources, experts, groups, capacity),
        out_shape=[shape((sources * rows, columns), F32), shape((sources, rows), F32)],
        in_specs=[VMEM] * (sources * groups + experts + sources + 1),
        out_specs=[VMEM] * 2,
        scratch_shapes=[pltpu.VMEM((sources, experts * capacity, columns), BF16)],
        compiler_params=params(),
        cost_estimate=cost(4 * sources * rows * experts * capacity * columns, 2 * experts * inner * columns),
        name="combine",
    )(*[hidden[g][m] for m in range(sources) for g in range(groups)], *downs, *metas, shared)

    peers = [squares] + [flip(squares, "tp", d) for d in range(1, sources)]
    gain = lax.dynamic_slice_in_dim(post_gain, tp[0] * columns, columns).reshape(1, columns)
    return pl.pallas_call(
        functools.partial(final_kernel, width),
        out_shape=shape((sources * rows, columns), BF16),
        in_specs=[SMEM] + [VMEM] * (2 + sources),
        out_specs=VMEM,
        compiler_params=params(),
        name="final",
    )(tp, combined, gain, *peers)


def plain(
    tokens, routes, gates, pre_gain, w_gate, w_up, w_down, sh_gate, sh_up, sh_down, post_gain, *, capacity
):
    tok_rows, full_width = tokens.shape
    experts_all = lax.axis_size("ep")
    inputs = tokens.astype(F32)
    scale_in = lax.rsqrt(jnp.mean(inputs * inputs, axis=1, keepdims=True) + EPS)
    normed = (inputs * scale_in * pre_gain[None, :]).astype(BF16)
    gate_shared = dot(normed, lax.all_gather(sh_gate, "tp", axis=0, tiled=True))
    up_shared = dot(normed, lax.all_gather(sh_up, "tp", axis=0, tiled=True))
    shared_hidden = (jax.nn.silu(gate_shared) * up_shared).astype(BF16)
    pair_count = tok_rows * TOPK
    expert_ids = routes.reshape(pair_count)
    matches = (expert_ids[:, None] == jnp.arange(experts_all, dtype=jnp.int32)[None, :]).astype(jnp.int32)
    earlier = jnp.cumsum(matches, axis=0) - matches
    dest_slot = expert_ids * capacity + jnp.sum(earlier * matches, axis=1)
    pair_token = jnp.arange(pair_count, dtype=jnp.int32) // TOPK
    slot_token = jnp.full((experts_all * capacity,), tok_rows, jnp.int32).at[dest_slot].set(pair_token)
    padded = jnp.concatenate([normed, jnp.zeros((1, full_width), BF16)], axis=0)
    outgoing = padded[slot_token].reshape(experts_all, capacity, full_width)
    arrived = lax.all_to_all(outgoing, "ep", split_axis=0, concat_axis=0, tiled=True)
    flat_rows = arrived.reshape(experts_all * capacity, full_width)
    hidden = (jax.nn.silu(dot(flat_rows, w_gate[0])) * dot(flat_rows, w_up[0])).astype(BF16)
    result = dot(hidden, w_down[0]).astype(BF16).reshape(arrived.shape)
    returned = lax.all_to_all(result, "ep", split_axis=0, concat_axis=0, tiled=True)
    picked = returned.reshape(experts_all * capacity, full_width)[dest_slot]
    weighted = picked.astype(F32) * gates.reshape(pair_count)[:, None]
    routed = jnp.sum(weighted.reshape(tok_rows, TOPK, full_width), axis=1).astype(BF16)
    shared = dot(shared_hidden, lax.all_gather(sh_down, "tp", axis=1, tiled=True)).astype(BF16)
    combined = routed.astype(F32) + shared.astype(F32)
    scale_out = lax.rsqrt(jnp.mean(combined * combined, axis=1, keepdims=True) + EPS)
    out_rows = (combined * scale_out * post_gain[None, :]).astype(BF16)
    return lax.all_to_all(out_rows, "tp", split_axis=1, concat_axis=0, tiled=True)


def per_device(tokens, *rest):
    experts, sources = lax.axis_size("ep"), lax.axis_size("tp")
    capacity = max(2, 4 * tokens.shape[0] * TOPK // (3 * experts))
    folds = experts & (experts - 1) == 0 and sources & (sources - 1) == 0 and min(experts, sources) > 1
    plan = folded if folds and capacity % 16 == 0 else plain
    return plan(tokens, *rest, capacity=capacity)


def solution(mesh):
    return jax.shard_map(
        per_device,
        mesh=mesh,
        in_specs=(
            P(("ep", "tp"), None),
            P(("ep", "tp"), None),
            P(("ep", "tp"), None),
            P(),
            P("ep", None, None),
            P("ep", None, None),
            P("ep", None, None),
            P("tp", None),
            P("tp", None),
            P(None, "tp"),
            P(),
        ),
        out_specs=P("ep", "tp"),
        check_vma=False,
    )
```

```python
import functools

import jax
import jax.numpy as jnp
from jax import lax
from jax.experimental import pallas as pl
from jax.experimental.pallas import tpu as pltpu
from jax.sharding import PartitionSpec as P


TOPK = 2
LANES = 128
EPS = 1e-06
F32, BF16 = jnp.float32, jnp.bfloat16
VMEM = pl.BlockSpec(memory_space=pltpu.VMEM)
SMEM = pl.BlockSpec(memory_space=pltpu.SMEM)
HBM = pl.BlockSpec(memory_space=pltpu.HBM)


def dot(a, b):
    return jnp.dot(a, b, preferred_element_type=F32)


def silu(v):
    return v / (1.0 + jnp.exp(-v))


def pre_kernel(capacity, me_ref, tok_in, routes_in, gates_in, gain_in, normed_ref, meta_ref, *refs):
    *bufs, tok, routes_ref, gates_ref, gain_ref, held, arrival, sent = refs
    experts = len(bufs)
    fetches = [
        pltpu.make_async_copy(source, target, arrival.at[i])
        for i, (source, target) in enumerate(
            [(routes_in, routes_ref), (tok_in, tok), (gain_in, gain_ref), (gates_in, gates_ref)]
        )
    ]
    for fetch in fetches:
        fetch.start()
    rows = tok.shape[0]
    fetches[0].wait()
    padded = -(-experts // 16) * 16
    rel = jnp.bitwise_xor(routes_ref[...], me_ref[0])
    first, second = rel[0:1], rel[1:2]
    expert = lax.broadcasted_iota(jnp.int32, (padded, rows), 0)
    hit0, hit1 = (first == expert).astype(F32), (second == expert).astype(F32)
    above = (
        lax.broadcasted_iota(jnp.int32, (rows, rows), 0)
        < lax.broadcasted_iota(jnp.int32, (rows, rows), 1)
    ).astype(F32).astype(BF16)
    before0 = dot(hit0.astype(BF16), above)
    before1 = dot(hit1.astype(BF16), above) + jnp.sum(hit0, axis=1, keepdims=True)
    slot0 = jnp.sum(before0 * hit0, axis=0, keepdims=True).astype(jnp.int32)
    slot1 = jnp.sum(before1 * hit1, axis=0, keepdims=True).astype(jnp.int32)
    dest0, dest1 = first * capacity + slot0, second * capacity + slot1
    meta_ref[...] = jnp.zeros_like(meta_ref)
    meta_ref[0:1] = dest0.astype(F32)
    meta_ref[1:2] = dest1.astype(F32)
    for fetch in fetches[1:]:
        fetch.wait()
    meta_ref[2:4] = gates_ref[...]
    x = tok[...].astype(F32)
    scale = lax.rsqrt(jnp.mean(x * x, axis=1, keepdims=True) + EPS)
    normed = (x * scale * gain_ref[...]).astype(BF16)
    normed_ref[...] = normed
    copies = []
    half = experts // 2
    for group in (range(half, experts), range(half)):
        low = group[0] * capacity
        place = lax.broadcasted_iota(jnp.int32, (half * capacity, rows), 0) + low
        chosen = ((place == dest0) | (place == dest1)).astype(F32).astype(BF16)
        held[low : low + half * capacity] = dot(chosen, normed).astype(BF16)
        for j in group:
            copy = pltpu.make_async_copy(held.at[pl.ds(j * capacity, capacity)], bufs[j], sent.at[j])
            copy.start()
            copies.append(copy)
    for copy in copies:
        copy.wait()


def gated_kernel(*refs):
    parts, (gate_ref, up_ref), out_ref = refs[:-3], refs[-3:-1], refs[-1]
    rows = jnp.concatenate([part[...] for part in parts], axis=0)
    gate, up = dot(rows, gate_ref[0]), dot(rows, up_ref[0])
    out_ref[...] = (silu(gate) * up).astype(BF16)


def shared_kernel(count, tp_ref, normed_ref, *refs):
    gates, ups, out_ref = refs[:count], refs[count : 2 * count], refs[-1]
    depth = gates[0].shape[0]
    gate = up = None
    for m in range(count):
        at = pl.multiple_of(jnp.bitwise_xor(tp_ref[0], m) * depth, depth)
        part = normed_ref[:, pl.ds(at, depth)]
        g, u = dot(part, gates[m][...]), dot(part, ups[m][...])
        gate, up = (g, u) if m == 0 else (gate + g, up + u)
    out_ref[...] = (silu(gate) * up).astype(BF16)


def shared_out_kernel(*refs):
    parts, down_ref, out_ref = refs[:-2], refs[-2], refs[-1]
    rows = parts[0].shape[0]
    for m, part in enumerate(parts):
        out_ref[m * rows : (m + 1) * rows] = dot(part[...], down_ref[...]).astype(BF16)


def combine_kernel(sources, sizes, capacity, *refs):
    groups, experts = len(sizes), sum(sizes)
    hidden = refs[: sources * groups]
    downs = refs[sources * groups : sources * groups + experts]
    metas = refs[sources * groups + experts : sources * groups + experts + sources]
    shared_ref, comb_ref, squares_ref, result = refs[-4:]
    j = 0
    for g, size in enumerate(sizes):
        for low in range(0, size * capacity, capacity):
            rows = jnp.concatenate(
                [hidden[g * sources + m][low : low + capacity] for m in range(sources)], axis=0
            )
            out = dot(rows, downs[j][...]).astype(BF16)
            for m in range(sources):
                result[m, j * capacity : (j + 1) * capacity] = out[m * capacity : (m + 1) * capacity]
            j += 1
    tokens = metas[0].shape[1]
    place = lax.broadcasted_iota(jnp.int32, (experts * capacity, tokens), 0)
    for m in range(sources):
        meta = metas[m][...]
        routed = None
        for k in range(TOPK):
            chosen = (place == meta[k : k + 1].astype(jnp.int32)).astype(F32).astype(BF16)
            picked = lax.dot_general(
                chosen, result[m], (((0,), (0,)), ((), ())), preferred_element_type=F32
            )
            gate = jnp.broadcast_to(meta[TOPK + k : TOPK + k + 1], (LANES, tokens)).T[:, 0:1]
            routed = picked * gate if k == 0 else routed + picked * gate
        here = slice(m * tokens, (m + 1) * tokens)
        combined = routed.astype(BF16).astype(F32) + shared_ref[here].astype(F32)
        comb_ref[here] = combined
        total = jnp.sum(combined * combined, axis=1, keepdims=True)
        squares_ref[m : m + 1] = jnp.broadcast_to(total, (tokens, LANES)).T[0:1]


def final_kernel(width, tp_ref, comb_ref, gain_ref, *refs):
    squares, out_ref = refs[:-1], refs[-1]
    count = len(squares)
    tokens = comb_ref.shape[0] // count
    gain = gain_ref[...]
    for m in range(count):
        total = squares[0][m : m + 1]
        for d in range(1, count):
            total = total + squares[d][m ^ d : (m ^ d) + 1]
        scale = lax.rsqrt(total / width + EPS)
        column = jnp.broadcast_to(scale, (LANES, tokens)).T[:, 0:1]
        at = pl.multiple_of(jnp.bitwise_xor(tp_ref[0], m) * tokens, 64)
        values = comb_ref[m * tokens : (m + 1) * tokens] * column * gain
        out_ref[pl.ds(at, tokens)] = values.astype(BF16)


def flip(value, axis, mask):
    size = lax.axis_size(axis)
    return lax.ppermute(value, axis, [(i, i ^ mask) for i in range(size)])


def gather_all(value, axis, steps=True):
    size = lax.axis_size(axis)
    held = {0: value}
    if not steps:
        return [value] + [flip(value, axis, j) for j in range(1, size)]
    mask = size // 2
    while mask:
        for j in list(held):
            held[j ^ mask] = flip(held[j], axis, mask)
        mask //= 2
    return [held[j] for j in range(size)]


def shape(dims, kind):
    return jax.ShapeDtypeStruct(dims, kind)


def call(kernel, out_shape, in_specs, out_specs, flops, moved, limit, scratch_shapes=()):
    def run(*operands):
        return pl.pallas_call(
            kernel,
            out_shape=out_shape,
            in_specs=in_specs,
            out_specs=out_specs,
            scratch_shapes=scratch_shapes,
            compiler_params=pltpu.CompilerParams(vmem_limit_bytes=limit * 2**20),
            cost_estimate=pl.CostEstimate(
                flops=int(flops), bytes_accessed=int(moved), transcendentals=0
            ),
        )(*operands)

    return run


def expert_groups(experts):
    near, quarter = experts // 2, experts // 4
    return [range(near), range(near, near + quarter), range(near + quarter, experts)]


def folded(
    tokens, routes, gates, pre_gain, w_gate, w_up, w_down, sh_gate, sh_up, sh_down, post_gain, *, capacity
):
    rows, width = tokens.shape
    experts, sources = lax.axis_size("ep"), lax.axis_size("tp")
    inner, columns = w_down.shape[1], width // sources
    ep = lax.axis_index("ep").astype(jnp.int32).reshape(1)
    tp = lax.axis_index("tp").astype(jnp.int32).reshape(1)
    groups = expert_groups(experts)

    own_down = lax.dynamic_slice_in_dim(w_down[0], tp[0] * columns, columns, axis=1)
    downs = gather_all(own_down, "ep")

    normed, meta, *bufs = call(
        functools.partial(pre_kernel, capacity),
        [shape((rows, width), BF16), shape((8, rows), F32)] + [shape((capacity, width), BF16)] * experts,
        [SMEM] + [HBM] * 4,
        [VMEM, VMEM] + [HBM] * experts,
        2 * rows * experts * capacity * width,
        4 * rows * width,
        60,
        [
            pltpu.VMEM((rows, width), BF16),
            pltpu.VMEM((TOPK, rows), jnp.int32),
            pltpu.VMEM((TOPK, rows), F32),
            pltpu.VMEM((1, width), F32),
            pltpu.VMEM((experts * capacity, width), BF16),
            pltpu.SemaphoreType.DMA((4,)),
            pltpu.SemaphoreType.DMA((experts,)),
        ],
    )(ep, tokens, routes.T, gates.T, pre_gain.reshape(1, width))

    arrived = [bufs[0]] + [flip(bufs[j], "ep", j) for j in range(1, experts)]

    sh_gates, sh_ups = gather_all(sh_gate, "tp"), gather_all(sh_up, "tp")
    metas = gather_all(meta, "tp", steps=False)

    shared_hidden = call(
        functools.partial(shared_kernel, sources),
        shape((rows, sh_down.shape[0]), BF16),
        [SMEM] + [VMEM] * (1 + 2 * sources),
        VMEM,
        4 * rows * width * inner,
        4 * width * inner,
        16,
    )(tp, normed, *sh_gates, *sh_ups)
    shared = call(
        shared_out_kernel,
        shape((sources * rows, columns), BF16),
        [VMEM] * (sources + 1),
        VMEM,
        2 * sources * rows * inner * columns,
        2 * inner * columns,
        16,
    )(*gather_all(shared_hidden, "tp"), sh_down)

    hidden = []
    for g, blocks in enumerate(groups):
        size = len(blocks)
        out = call(
            gated_kernel,
            shape((size * capacity, inner), BF16),
            [VMEM] * (size + 2),
            VMEM,
            4 * size * capacity * width * inner,
            4 * width * inner,
            16,
        )(*[arrived[j] for j in blocks], w_gate, w_up)
        back = []
        for b, j in enumerate(blocks):
            block = out[b * capacity : (b + 1) * capacity]
            back.append(block if j == 0 else flip(block, "ep", j))
        hidden += gather_all(jnp.concatenate(back, axis=0), "tp", steps=g < len(groups) - 1)

    combined, squares = call(
        functools.partial(combine_kernel, sources, [len(blocks) for blocks in groups], capacity),
        [shape((sources * rows, columns), F32), shape((sources, rows), F32)],
        [VMEM] * (len(hidden) + experts + sources + 1),
        [VMEM] * 2,
        4 * sources * rows * experts * capacity * columns,
        2 * experts * inner * columns,
        24,
        [pltpu.VMEM((sources, experts * capacity, columns), BF16)],
    )(*hidden, *downs, *metas, shared)

    gain = lax.dynamic_slice_in_dim(post_gain, tp[0] * columns, columns).reshape(1, columns)
    return call(
        functools.partial(final_kernel, width),
        shape((sources * rows, columns), BF16),
        [SMEM] + [VMEM] * (2 + sources),
        VMEM,
        8 * sources * rows * columns,
        6 * sources * rows * columns,
        16,
    )(tp, combined, gain, *gather_all(squares, "tp", steps=False))


def plain(
    tokens, routes, gates, pre_gain, w_gate, w_up, w_down, sh_gate, sh_up, sh_down, post_gain, *, capacity
):
    tok_rows, full_width = tokens.shape
    experts_all = lax.axis_size("ep")
    inputs = tokens.astype(F32)
    scale_in = lax.rsqrt(jnp.mean(inputs * inputs, axis=1, keepdims=True) + EPS)
    normed = (inputs * scale_in * pre_gain[None, :]).astype(BF16)
    gate_shared = dot(normed, lax.all_gather(sh_gate, "tp", axis=0, tiled=True))
    up_shared = dot(normed, lax.all_gather(sh_up, "tp", axis=0, tiled=True))
    shared_hidden = (jax.nn.silu(gate_shared) * up_shared).astype(BF16)
    pair_count = tok_rows * TOPK
    expert_ids = routes.reshape(pair_count)
    matches = (expert_ids[:, None] == jnp.arange(experts_all, dtype=jnp.int32)[None, :]).astype(jnp.int32)
    earlier = jnp.cumsum(matches, axis=0) - matches
    dest_slot = expert_ids * capacity + jnp.sum(earlier * matches, axis=1)
    pair_token = jnp.arange(pair_count, dtype=jnp.int32) // TOPK
    slot_token = jnp.full((experts_all * capacity,), tok_rows, jnp.int32).at[dest_slot].set(pair_token)
    padded = jnp.concatenate([normed, jnp.zeros((1, full_width), BF16)], axis=0)
    outgoing = padded[slot_token].reshape(experts_all, capacity, full_width)
    arrived = lax.all_to_all(outgoing, "ep", split_axis=0, concat_axis=0, tiled=True)
    flat_rows = arrived.reshape(experts_all * capacity, full_width)
    hidden = (jax.nn.silu(dot(flat_rows, w_gate[0])) * dot(flat_rows, w_up[0])).astype(BF16)
    result = dot(hidden, w_down[0]).astype(BF16).reshape(arrived.shape)
    returned = lax.all_to_all(result, "ep", split_axis=0, concat_axis=0, tiled=True)
    picked = returned.reshape(experts_all * capacity, full_width)[dest_slot]
    weighted = picked.astype(F32) * gates.reshape(pair_count)[:, None]
    routed = jnp.sum(weighted.reshape(tok_rows, TOPK, full_width), axis=1).astype(BF16)
    shared = dot(shared_hidden, lax.all_gather(sh_down, "tp", axis=1, tiled=True)).astype(BF16)
    combined = routed.astype(F32) + shared.astype(F32)
    scale_out = lax.rsqrt(jnp.mean(combined * combined, axis=1, keepdims=True) + EPS)
    out_rows = (combined * scale_out * post_gain[None, :]).astype(BF16)
    return lax.all_to_all(out_rows, "tp", split_axis=1, concat_axis=0, tiled=True)


def folds(experts, sources):
    powers = experts & (experts - 1) == 0 and sources & (sources - 1) == 0
    return powers and experts >= 4 and sources >= 2


def per_device(tokens, *rest):
    experts, sources = lax.axis_size("ep"), lax.axis_size("tp")
    plan = folded if folds(experts, sources) else plain
    capacity = max(2, 4 * tokens.shape[0] * TOPK // (3 * experts))
    return plan(tokens, *rest, capacity=capacity)


def solution(mesh):
    return jax.shard_map(
        per_device,
        mesh=mesh,
        in_specs=(
            P(("ep", "tp"), None),
            P(("ep", "tp"), None),
            P(("ep", "tp"), None),
            P(),
            P("ep", None, None),
            P("ep", None, None),
            P("ep", None, None),
            P("tp", None),
            P("tp", None),
            P(None, "tp"),
            P(),
        ),
        out_specs=P("ep", "tp"),
        check_vma=False,
    )
```

```python
import functools

import jax
import jax.numpy as jnp
from jax import lax
from jax.experimental import pallas as pl
from jax.experimental.pallas import tpu as pltpu
from jax.sharding import PartitionSpec as P


TOPK = 2
LANES = 128
EPS = 1e-06
F32, BF16 = jnp.float32, jnp.bfloat16
VMEM = pl.BlockSpec(memory_space=pltpu.VMEM)
SMEM = pl.BlockSpec(memory_space=pltpu.SMEM)
HBM = pl.BlockSpec(memory_space=pltpu.HBM)


def dot(a, b):
    return jnp.dot(a, b, preferred_element_type=F32)


def silu(v):
    return v / (1.0 + jnp.exp(-v))


def pre_kernel(capacity, me_ref, tok_in, routes_in, gates_in, gain_in, normed_ref, meta_ref, *refs):
    *bufs, tok, routes_ref, gates_ref, gain_ref, held, arrival, sent = refs
    experts = len(bufs)
    fetches = [
        pltpu.make_async_copy(source, target, arrival.at[i])
        for i, (source, target) in enumerate(
            [(routes_in, routes_ref), (tok_in, tok), (gain_in, gain_ref), (gates_in, gates_ref)]
        )
    ]
    for fetch in fetches:
        fetch.start()
    rows = tok.shape[0]
    fetches[0].wait()
    padded = -(-experts // 16) * 16
    rel = jnp.bitwise_xor(routes_ref[...], me_ref[0])
    first, second = rel[0:1], rel[1:2]
    expert = lax.broadcasted_iota(jnp.int32, (padded, rows), 0)
    hit0, hit1 = (first == expert).astype(F32), (second == expert).astype(F32)
    above = (
        lax.broadcasted_iota(jnp.int32, (rows, rows), 0)
        < lax.broadcasted_iota(jnp.int32, (rows, rows), 1)
    ).astype(F32).astype(BF16)
    before0 = dot(hit0.astype(BF16), above)
    before1 = dot(hit1.astype(BF16), above) + jnp.sum(hit0, axis=1, keepdims=True)
    slot0 = jnp.sum(before0 * hit0, axis=0, keepdims=True).astype(jnp.int32)
    slot1 = jnp.sum(before1 * hit1, axis=0, keepdims=True).astype(jnp.int32)
    dest0, dest1 = first * capacity + slot0, second * capacity + slot1
    meta_ref[...] = jnp.zeros_like(meta_ref)
    meta_ref[0:1] = dest0.astype(F32)
    meta_ref[1:2] = dest1.astype(F32)
    for fetch in fetches[1:]:
        fetch.wait()
    meta_ref[2:4] = gates_ref[...]
    x = tok[...].astype(F32)
    scale = lax.rsqrt(jnp.mean(x * x, axis=1, keepdims=True) + EPS)
    normed = (x * scale * gain_ref[...]).astype(BF16)
    normed_ref[...] = normed
    copies = []
    half = experts // 2
    for group in (range(half, experts), range(half)):
        low = group[0] * capacity
        place = lax.broadcasted_iota(jnp.int32, (half * capacity, rows), 0) + low
        chosen = ((place == dest0) | (place == dest1)).astype(F32).astype(BF16)
        held[low : low + half * capacity] = dot(chosen, normed).astype(BF16)
        for j in group:
            copy = pltpu.make_async_copy(held.at[pl.ds(j * capacity, capacity)], bufs[j], sent.at[j])
            copy.start()
            copies.append(copy)
    for copy in copies:
        copy.wait()


def gated_kernel(*refs):
    parts, (gate_ref, up_ref), out_ref = refs[:-3], refs[-3:-1], refs[-1]
    rows = jnp.concatenate([part[...] for part in parts], axis=0)
    gate, up = dot(rows, gate_ref[0]), dot(rows, up_ref[0])
    out_ref[...] = (silu(gate) * up).astype(BF16)


def shared_kernel(count, tp_ref, normed_ref, *refs):
    gates, ups, out_ref = refs[:count], refs[count : 2 * count], refs[-1]
    depth = gates[0].shape[0]
    gate = up = None
    for m in range(count):
        at = pl.multiple_of(jnp.bitwise_xor(tp_ref[0], m) * depth, depth)
        part = normed_ref[:, pl.ds(at, depth)]
        g, u = dot(part, gates[m][...]), dot(part, ups[m][...])
        gate, up = (g, u) if m == 0 else (gate + g, up + u)
    out_ref[...] = (silu(gate) * up).astype(BF16)


def shared_out_kernel(*refs):
    parts, down_ref, out_ref = refs[:-2], refs[-2], refs[-1]
    rows = parts[0].shape[0]
    for m, part in enumerate(parts):
        out_ref[m * rows : (m + 1) * rows] = dot(part[...], down_ref[...]).astype(BF16)


def weighted(sources, sizes, first, capacity, refs, result, sums):
    groups, experts = len(sizes), sum(sizes)
    hidden = refs[: sources * groups]
    downs = refs[sources * groups : sources * groups + experts]
    metas = refs[sources * groups + experts : sources * groups + experts + sources]
    j = 0
    for g, size in enumerate(sizes):
        for low in range(0, size * capacity, capacity):
            rows = jnp.concatenate(
                [hidden[g * sources + m][low : low + capacity] for m in range(sources)], axis=0
            )
            out = dot(rows, downs[j][...]).astype(BF16)
            for m in range(sources):
                result[m, j * capacity : (j + 1) * capacity] = out[m * capacity : (m + 1) * capacity]
            j += 1
    tokens = metas[0].shape[1]
    place = lax.broadcasted_iota(jnp.int32, (experts * capacity, tokens), 0) + first * capacity
    for m in range(sources):
        meta = metas[m][...]
        total = None if sums is None else sums[m * tokens : (m + 1) * tokens]
        for k in range(TOPK):
            chosen = (place == meta[k : k + 1].astype(jnp.int32)).astype(F32).astype(BF16)
            picked = lax.dot_general(
                chosen, result[m], (((0,), (0,)), ((), ())), preferred_element_type=F32
            )
            gate = jnp.broadcast_to(meta[TOPK + k : TOPK + k + 1], (LANES, tokens)).T[:, 0:1]
            total = picked * gate if total is None else total + picked * gate
        yield m, slice(m * tokens, (m + 1) * tokens), total


def early_kernel(sources, sizes, capacity, *refs):
    sums_ref, result = refs[-2:]
    for _, here, total in weighted(sources, sizes, 0, capacity, refs, result, None):
        sums_ref[here] = total


def late_kernel(sources, sizes, first, capacity, *refs):
    sums_ref, shared_ref, comb_ref, squares_ref, result = refs[-5:]
    for m, here, total in weighted(sources, sizes, first, capacity, refs, result, sums_ref):
        combined = total.astype(BF16).astype(F32) + shared_ref[here].astype(F32)
        comb_ref[here] = combined
        squares = jnp.sum(combined * combined, axis=1, keepdims=True)
        squares_ref[m : m + 1] = jnp.broadcast_to(squares, (combined.shape[0], LANES)).T[0:1]


def final_kernel(width, tp_ref, comb_ref, gain_ref, *refs):
    squares, out_ref = refs[:-1], refs[-1]
    count = len(squares)
    tokens = comb_ref.shape[0] // count
    gain = gain_ref[...]
    for m in range(count):
        total = squares[0][m : m + 1]
        for d in range(1, count):
            total = total + squares[d][m ^ d : (m ^ d) + 1]
        scale = lax.rsqrt(total / width + EPS)
        column = jnp.broadcast_to(scale, (LANES, tokens)).T[:, 0:1]
        at = pl.multiple_of(jnp.bitwise_xor(tp_ref[0], m) * tokens, 64)
        values = comb_ref[m * tokens : (m + 1) * tokens] * column * gain
        out_ref[pl.ds(at, tokens)] = values.astype(BF16)


def flip(value, axis, mask):
    size = lax.axis_size(axis)
    return lax.ppermute(value, axis, [(i, i ^ mask) for i in range(size)])


def gather_all(value, axis, steps=True):
    size = lax.axis_size(axis)
    held = {0: value}
    if not steps:
        return [value] + [flip(value, axis, j) for j in range(1, size)]
    mask = size // 2
    while mask:
        for j in list(held):
            held[j ^ mask] = flip(held[j], axis, mask)
        mask //= 2
    return [held[j] for j in range(size)]


def shape(dims, kind):
    return jax.ShapeDtypeStruct(dims, kind)


def call(kernel, out_shape, in_specs, out_specs, flops, moved, limit, scratch_shapes=()):
    def run(*operands):
        return pl.pallas_call(
            kernel,
            out_shape=out_shape,
            in_specs=in_specs,
            out_specs=out_specs,
            scratch_shapes=scratch_shapes,
            compiler_params=pltpu.CompilerParams(vmem_limit_bytes=limit * 2**20),
            cost_estimate=pl.CostEstimate(
                flops=int(flops), bytes_accessed=int(moved), transcendentals=0
            ),
        )(*operands)

    return run


def expert_groups(experts):
    near, quarter = experts // 2, experts // 4
    return [range(near), range(near, near + quarter), range(near + quarter, experts)]


def folded(
    tokens, routes, gates, pre_gain, w_gate, w_up, w_down, sh_gate, sh_up, sh_down, post_gain, *, capacity
):
    rows, width = tokens.shape
    experts, sources = lax.axis_size("ep"), lax.axis_size("tp")
    inner, columns = w_down.shape[1], width // sources
    ep = lax.axis_index("ep").astype(jnp.int32).reshape(1)
    tp = lax.axis_index("tp").astype(jnp.int32).reshape(1)
    groups = expert_groups(experts)

    own_down = lax.dynamic_slice_in_dim(w_down[0], tp[0] * columns, columns, axis=1)
    downs = gather_all(own_down, "ep")

    normed, meta, *bufs = call(
        functools.partial(pre_kernel, capacity),
        [shape((rows, width), BF16), shape((8, rows), F32)] + [shape((capacity, width), BF16)] * experts,
        [SMEM] + [HBM] * 4,
        [VMEM, VMEM] + [HBM] * experts,
        2 * rows * experts * capacity * width,
        4 * rows * width,
        60,
        [
            pltpu.VMEM((rows, width), BF16),
            pltpu.VMEM((TOPK, rows), jnp.int32),
            pltpu.VMEM((TOPK, rows), F32),
            pltpu.VMEM((1, width), F32),
            pltpu.VMEM((experts * capacity, width), BF16),
            pltpu.SemaphoreType.DMA((4,)),
            pltpu.SemaphoreType.DMA((experts,)),
        ],
    )(ep, tokens, routes.T, gates.T, pre_gain.reshape(1, width))

    arrived = [bufs[0]] + [flip(bufs[j], "ep", j) for j in range(1, experts)]

    sh_gates, sh_ups = gather_all(sh_gate, "tp"), gather_all(sh_up, "tp")
    metas = gather_all(meta, "tp", steps=False)

    shared_hidden = call(
        functools.partial(shared_kernel, sources),
        shape((rows, sh_down.shape[0]), BF16),
        [SMEM] + [VMEM] * (1 + 2 * sources),
        VMEM,
        4 * rows * width * inner,
        4 * width * inner,
        16,
    )(tp, normed, *sh_gates, *sh_ups)
    shared = call(
        shared_out_kernel,
        shape((sources * rows, columns), BF16),
        [VMEM] * (sources + 1),
        VMEM,
        2 * sources * rows * inner * columns,
        2 * inner * columns,
        16,
    )(*gather_all(shared_hidden, "tp"), sh_down)

    hidden = []
    for g, blocks in enumerate(groups):
        size = len(blocks)
        out = call(
            gated_kernel,
            shape((size * capacity, inner), BF16),
            [VMEM] * (size + 2),
            VMEM,
            4 * size * capacity * width * inner,
            4 * width * inner,
            16,
        )(*[arrived[j] for j in blocks], w_gate, w_up)
        back = []
        for b, j in enumerate(blocks):
            block = out[b * capacity : (b + 1) * capacity]
            back.append(block if j == 0 else flip(block, "ep", j))
        hidden += gather_all(jnp.concatenate(back, axis=0), "tp", steps=g < len(groups) - 1)

    def weighing(kernel, sizes, first, outs, extra, *operands):
        count = len(operands) - extra
        slots = sum(sizes) * capacity
        return call(
            functools.partial(kernel, sources, sizes, *first, capacity),
            outs,
            [VMEM] * len(operands),
            [VMEM] * len(outs),
            4 * sources * rows * slots * columns,
            2 * count * inner * columns,
            24,
            [pltpu.VMEM((sources, slots, columns), BF16)],
        )(*operands)

    sizes, last = [len(blocks) for blocks in groups], experts - len(groups[-1])
    result = shape((sources * rows, columns), F32)
    (sums,) = weighing(early_kernel, sizes[:-1], (), [result], 0, *hidden[:-sources], *downs[:last], *metas)
    combined, squares = weighing(
        late_kernel,
        sizes[-1:],
        (last,),
        [result, shape((sources, rows), F32)],
        2,
        *hidden[-sources:],
        *downs[last:],
        *metas,
        sums,
        shared,
    )

    gain = lax.dynamic_slice_in_dim(post_gain, tp[0] * columns, columns).reshape(1, columns)
    return call(
        functools.partial(final_kernel, width),
        shape((sources * rows, columns), BF16),
        [SMEM] + [VMEM] * (2 + sources),
        VMEM,
        8 * sources * rows * columns,
        6 * sources * rows * columns,
        16,
    )(tp, combined, gain, *gather_all(squares, "tp", steps=False))


def plain(
    tokens, routes, gates, pre_gain, w_gate, w_up, w_down, sh_gate, sh_up, sh_down, post_gain, *, capacity
):
    tok_rows, full_width = tokens.shape
    experts_all = lax.axis_size("ep")
    inputs = tokens.astype(F32)
    scale_in = lax.rsqrt(jnp.mean(inputs * inputs, axis=1, keepdims=True) + EPS)
    normed = (inputs * scale_in * pre_gain[None, :]).astype(BF16)
    gate_shared = dot(normed, lax.all_gather(sh_gate, "tp", axis=0, tiled=True))
    up_shared = dot(normed, lax.all_gather(sh_up, "tp", axis=0, tiled=True))
    shared_hidden = (jax.nn.silu(gate_shared) * up_shared).astype(BF16)
    pair_count = tok_rows * TOPK
    expert_ids = routes.reshape(pair_count)
    matches = (expert_ids[:, None] == jnp.arange(experts_all, dtype=jnp.int32)[None, :]).astype(jnp.int32)
    earlier = jnp.cumsum(matches, axis=0) - matches
    dest_slot = expert_ids * capacity + jnp.sum(earlier * matches, axis=1)
    pair_token = jnp.arange(pair_count, dtype=jnp.int32) // TOPK
    slot_token = jnp.full((experts_all * capacity,), tok_rows, jnp.int32).at[dest_slot].set(pair_token)
    padded = jnp.concatenate([normed, jnp.zeros((1, full_width), BF16)], axis=0)
    outgoing = padded[slot_token].reshape(experts_all, capacity, full_width)
    arrived = lax.all_to_all(outgoing, "ep", split_axis=0, concat_axis=0, tiled=True)
    flat_rows = arrived.reshape(experts_all * capacity, full_width)
    hidden = (jax.nn.silu(dot(flat_rows, w_gate[0])) * dot(flat_rows, w_up[0])).astype(BF16)
    result = dot(hidden, w_down[0]).astype(BF16).reshape(arrived.shape)
    returned = lax.all_to_all(result, "ep", split_axis=0, concat_axis=0, tiled=True)
    picked = returned.reshape(experts_all * capacity, full_width)[dest_slot]
    weighted = picked.astype(F32) * gates.reshape(pair_count)[:, None]
    routed = jnp.sum(weighted.reshape(tok_rows, TOPK, full_width), axis=1).astype(BF16)
    shared = dot(shared_hidden, lax.all_gather(sh_down, "tp", axis=1, tiled=True)).astype(BF16)
    combined = routed.astype(F32) + shared.astype(F32)
    scale_out = lax.rsqrt(jnp.mean(combined * combined, axis=1, keepdims=True) + EPS)
    out_rows = (combined * scale_out * post_gain[None, :]).astype(BF16)
    return lax.all_to_all(out_rows, "tp", split_axis=1, concat_axis=0, tiled=True)


def folds(experts, sources):
    powers = experts & (experts - 1) == 0 and sources & (sources - 1) == 0
    return powers and experts >= 4 and sources >= 2


def per_device(tokens, *rest):
    experts, sources = lax.axis_size("ep"), lax.axis_size("tp")
    plan = folded if folds(experts, sources) else plain
    capacity = max(2, 4 * tokens.shape[0] * TOPK // (3 * experts))
    return plan(tokens, *rest, capacity=capacity)


def solution(mesh):
    return jax.shard_map(
        per_device,
        mesh=mesh,
        in_specs=(
            P(("ep", "tp"), None),
            P(("ep", "tp"), None),
            P(("ep", "tp"), None),
            P(),
            P("ep", None, None),
            P("ep", None, None),
            P("ep", None, None),
            P("tp", None),
            P("tp", None),
            P(None, "tp"),
            P(),
        ),
        out_specs=P("ep", "tp"),
        check_vma=False,
    )
```

```python
import functools

import jax
import jax.numpy as jnp
from jax import lax
from jax.experimental import pallas as pl
from jax.experimental.pallas import tpu as pltpu
from jax.sharding import PartitionSpec as P


TOPK = 2
LANES = 128
EPS = 1e-06
F32, BF16 = jnp.float32, jnp.bfloat16
VMEM = pl.BlockSpec(memory_space=pltpu.VMEM)
SMEM = pl.BlockSpec(memory_space=pltpu.SMEM)
HBM = pl.BlockSpec(memory_space=pltpu.HBM)


def dot(a, b):
    return jnp.dot(a, b, preferred_element_type=F32)


def silu(v):
    return v / (1.0 + jnp.exp(-v))


def pre_kernel(capacity, me_ref, tok_in, routes_in, gates_in, gain_in, normed_ref, meta_ref, *refs):
    *bufs, tok, routes_ref, gates_ref, gain_ref, held, arrival, sent = refs
    experts = len(bufs)
    fetches = [
        pltpu.make_async_copy(source, target, arrival.at[i])
        for i, (source, target) in enumerate(
            [(routes_in, routes_ref), (tok_in, tok), (gain_in, gain_ref), (gates_in, gates_ref)]
        )
    ]
    for fetch in fetches:
        fetch.start()
    rows = tok.shape[0]
    fetches[0].wait()
    padded = -(-experts // 16) * 16
    rel = jnp.bitwise_xor(routes_ref[...], me_ref[0])
    first, second = rel[0:1], rel[1:2]
    expert = lax.broadcasted_iota(jnp.int32, (padded, rows), 0)
    hit0, hit1 = (first == expert).astype(F32), (second == expert).astype(F32)
    above = (
        lax.broadcasted_iota(jnp.int32, (rows, rows), 0)
        < lax.broadcasted_iota(jnp.int32, (rows, rows), 1)
    ).astype(F32).astype(BF16)
    before0 = dot(hit0.astype(BF16), above)
    before1 = dot(hit1.astype(BF16), above) + jnp.sum(hit0, axis=1, keepdims=True)
    slot0 = jnp.sum(before0 * hit0, axis=0, keepdims=True).astype(jnp.int32)
    slot1 = jnp.sum(before1 * hit1, axis=0, keepdims=True).astype(jnp.int32)
    dest0, dest1 = first * capacity + slot0, second * capacity + slot1
    meta_ref[...] = jnp.zeros_like(meta_ref)
    meta_ref[0:1] = dest0.astype(F32)
    meta_ref[1:2] = dest1.astype(F32)
    for fetch in fetches[1:]:
        fetch.wait()
    meta_ref[2:4] = gates_ref[...]
    x = tok[...].astype(F32)
    scale = lax.rsqrt(jnp.mean(x * x, axis=1, keepdims=True) + EPS)
    normed = (x * scale * gain_ref[...]).astype(BF16)
    normed_ref[...] = normed
    copies = []
    half = experts // 2
    for group in (range(half, experts), range(half)):
        low = group[0] * capacity
        place = lax.broadcasted_iota(jnp.int32, (half * capacity, rows), 0) + low
        chosen = ((place == dest0) | (place == dest1)).astype(F32).astype(BF16)
        held[low : low + half * capacity] = dot(chosen, normed).astype(BF16)
        for j in group:
            copy = pltpu.make_async_copy(held.at[pl.ds(j * capacity, capacity)], bufs[j], sent.at[j])
            copy.start()
            copies.append(copy)
    for copy in copies:
        copy.wait()


def gated_kernel(*refs):
    parts, (gate_ref, up_ref), out_ref = refs[:-3], refs[-3:-1], refs[-1]
    rows = jnp.concatenate([part[...] for part in parts], axis=0)
    gate, up = dot(rows, gate_ref[0]), dot(rows, up_ref[0])
    out_ref[...] = (silu(gate) * up).astype(BF16)


def shared_kernel(count, tp_ref, normed_ref, *refs):
    gates, ups, out_ref = refs[:count], refs[count : 2 * count], refs[-1]
    depth = gates[0].shape[0]
    gate = up = None
    for m in range(count):
        at = pl.multiple_of(jnp.bitwise_xor(tp_ref[0], m) * depth, depth)
        part = normed_ref[:, pl.ds(at, depth)]
        g, u = dot(part, gates[m][...]), dot(part, ups[m][...])
        gate, up = (g, u) if m == 0 else (gate + g, up + u)
    out_ref[...] = (silu(gate) * up).astype(BF16)


def shared_out_kernel(*refs):
    parts, down_ref, out_ref = refs[:-2], refs[-2], refs[-1]
    rows = parts[0].shape[0]
    for m, part in enumerate(parts):
        out_ref[m * rows : (m + 1) * rows] = dot(part[...], down_ref[...]).astype(BF16)


def column(row, rows):
    return jnp.broadcast_to(row, (LANES, rows)).T[:, 0:1]


def choices(meta, first, slots):
    place = lax.broadcasted_iota(jnp.int32, (slots, meta.shape[1]), 0) + first
    return [
        (place == meta[k : k + 1].astype(jnp.int32)).astype(F32).astype(BF16) for k in range(TOPK)
    ]


def project(parts, down, result, at, capacity):
    out = dot(jnp.concatenate(parts, axis=0), down).astype(BF16)
    for m in range(len(parts)):
        result[m, at : at + capacity] = out[m * capacity : (m + 1) * capacity]


def weighted(chosen, meta, rows):
    total = None
    for k in range(TOPK):
        picked = lax.dot_general(chosen[k], rows, (((0,), (0,)), ((), ())), preferred_element_type=F32)
        term = picked * column(meta[TOPK + k : TOPK + k + 1], meta.shape[1])
        total = term if total is None else total + term
    return total


def early_kernel(sources, sizes, capacity, *refs):
    groups, experts = len(sizes), sum(sizes)
    hidden = refs[: sources * groups]
    downs = refs[sources * groups : sources * groups + experts]
    metas, sums_ref, result = refs[sources * groups + experts : -2], refs[-2], refs[-1]
    j = 0
    for g, size in enumerate(sizes):
        for low in range(0, size * capacity, capacity):
            parts = [hidden[g * sources + m][low : low + capacity] for m in range(sources)]
            project(parts, downs[j][...], result, j * capacity, capacity)
            j += 1
    for m in range(sources):
        meta = metas[m][...]
        tokens = meta.shape[1]
        chosen = choices(meta, 0, experts * capacity)
        sums_ref[m * tokens : (m + 1) * tokens] = weighted(chosen, meta, result[m])


def late_kernel(sources, experts, first, capacity, *refs):
    hidden, downs = refs[:sources], refs[sources : sources + experts]
    metas, (shared_ref, sums_ref) = refs[sources + experts : -5], refs[-5:-3]
    comb_ref, squares_ref, result = refs[-3:]
    for j in range(experts):
        at = j * capacity
        project([part[at : at + capacity] for part in hidden], downs[j][...], result, at, capacity)
    for m in range(sources):
        meta = metas[m][...]
        tokens = meta.shape[1]
        here = slice(m * tokens, (m + 1) * tokens)
        chosen = choices(meta, first * capacity, experts * capacity)
        routed = sums_ref[here] + weighted(chosen, meta, result[m])
        combined = routed.astype(BF16).astype(F32) + shared_ref[here].astype(F32)
        comb_ref[here] = combined
        squares = jnp.sum(combined * combined, axis=1, keepdims=True)
        squares_ref[m : m + 1] = jnp.broadcast_to(squares, (tokens, LANES)).T[0:1]


def final_kernel(width, tp_ref, comb_ref, gain_ref, *refs):
    *squares, out_ref, held, sent = refs
    count = len(squares)
    tokens = comb_ref.shape[0] // count
    gain = gain_ref[...]
    copies = []
    for m in range(count):
        total = squares[0][m : m + 1]
        for d in range(1, count):
            total = total + squares[d][m ^ d : (m ^ d) + 1]
        scale = column(lax.rsqrt(total / width + EPS), tokens)
        here = slice(m * tokens, (m + 1) * tokens)
        held[here] = (comb_ref[here] * scale * gain).astype(BF16)
        at = pl.multiple_of(jnp.bitwise_xor(tp_ref[0], m) * tokens, 64)
        copy = pltpu.make_async_copy(
            held.at[pl.ds(m * tokens, tokens)], out_ref.at[pl.ds(at, tokens)], sent.at[m]
        )
        copy.start()
        copies.append(copy)
    for copy in copies:
        copy.wait()


def flip(value, axis, mask):
    size = lax.axis_size(axis)
    return lax.ppermute(value, axis, [(i, i ^ mask) for i in range(size)])


def gather_all(value, axis, steps=True):
    size = lax.axis_size(axis)
    held = {0: value}
    if not steps:
        return [value] + [flip(value, axis, j) for j in range(1, size)]
    mask = size // 2
    while mask:
        for j in list(held):
            held[j ^ mask] = flip(held[j], axis, mask)
        mask //= 2
    return [held[j] for j in range(size)]


def shape(dims, kind):
    return jax.ShapeDtypeStruct(dims, kind)


def call(kernel, out_shape, in_specs, out_specs, flops, moved, limit, scratch_shapes=()):
    def run(*operands):
        return pl.pallas_call(
            kernel,
            out_shape=out_shape,
            in_specs=in_specs,
            out_specs=out_specs,
            scratch_shapes=scratch_shapes,
            compiler_params=pltpu.CompilerParams(vmem_limit_bytes=limit * 2**20),
            cost_estimate=pl.CostEstimate(
                flops=int(flops), bytes_accessed=int(moved), transcendentals=0
            ),
        )(*operands)

    return run


def expert_groups(experts):
    near, quarter = experts // 2, experts // 4
    return [range(near), range(near, near + quarter), range(near + quarter, experts)]


def folded(
    tokens, routes, gates, pre_gain, w_gate, w_up, w_down, sh_gate, sh_up, sh_down, post_gain, *, capacity
):
    rows, width = tokens.shape
    experts, sources = lax.axis_size("ep"), lax.axis_size("tp")
    inner, columns = w_down.shape[1], width // sources
    ep = lax.axis_index("ep").astype(jnp.int32).reshape(1)
    tp = lax.axis_index("tp").astype(jnp.int32).reshape(1)
    groups = expert_groups(experts)

    own_down = lax.dynamic_slice_in_dim(w_down[0], tp[0] * columns, columns, axis=1)
    downs = gather_all(own_down, "ep")

    normed, meta, *bufs = call(
        functools.partial(pre_kernel, capacity),
        [shape((rows, width), BF16), shape((8, rows), F32)] + [shape((capacity, width), BF16)] * experts,
        [SMEM] + [HBM] * 4,
        [VMEM, VMEM] + [HBM] * experts,
        2 * rows * experts * capacity * width,
        4 * rows * width,
        60,
        [
            pltpu.VMEM((rows, width), BF16),
            pltpu.VMEM((TOPK, rows), jnp.int32),
            pltpu.VMEM((TOPK, rows), F32),
            pltpu.VMEM((1, width), F32),
            pltpu.VMEM((experts * capacity, width), BF16),
            pltpu.SemaphoreType.DMA((4,)),
            pltpu.SemaphoreType.DMA((experts,)),
        ],
    )(ep, tokens, routes.T, gates.T, pre_gain.reshape(1, width))

    arrived = [bufs[0]] + [flip(bufs[j], "ep", j) for j in range(1, experts)]

    sh_gates, sh_ups = gather_all(sh_gate, "tp"), gather_all(sh_up, "tp")
    metas = gather_all(meta, "tp", steps=False)

    shared_hidden = call(
        functools.partial(shared_kernel, sources),
        shape((rows, sh_down.shape[0]), BF16),
        [SMEM] + [VMEM] * (1 + 2 * sources),
        VMEM,
        4 * rows * width * inner,
        4 * width * inner,
        16,
    )(tp, normed, *sh_gates, *sh_ups)
    shared = call(
        shared_out_kernel,
        shape((sources * rows, columns), BF16),
        [VMEM] * (sources + 1),
        VMEM,
        2 * sources * rows * inner * columns,
        2 * inner * columns,
        16,
    )(*gather_all(shared_hidden, "tp"), sh_down)

    hidden = []
    for blocks in groups:
        size = len(blocks)
        out = call(
            gated_kernel,
            shape((size * capacity, inner), BF16),
            [VMEM] * (size + 2),
            VMEM,
            4 * size * capacity * width * inner,
            4 * width * inner,
            16,
        )(*[arrived[j] for j in blocks], w_gate, w_up)
        back = []
        for b, j in enumerate(blocks):
            block = out[b * capacity : (b + 1) * capacity]
            back.append(block if j == 0 else flip(block, "ep", j))
        hidden += gather_all(jnp.concatenate(back, axis=0), "tp")

    sizes, last = [len(blocks) for blocks in groups], experts - len(groups[-1])
    sums_shape = shape((sources * rows, columns), F32)
    slots, rest = last * capacity, sizes[-1] * capacity
    sums = call(
        functools.partial(early_kernel, sources, sizes[:-1], capacity),
        sums_shape,
        [VMEM] * (len(hidden) - sources + last + sources),
        VMEM,
        4 * sources * rows * slots * columns,
        2 * last * inner * columns,
        24,
        [pltpu.VMEM((sources, slots, columns), BF16)],
    )(*hidden[:-sources], *downs[:last], *metas)
    combined, squares = call(
        functools.partial(late_kernel, sources, sizes[-1], last, capacity),
        [sums_shape, shape((sources, rows), F32)],
        [VMEM] * (2 * sources + sizes[-1] + 2),
        [VMEM] * 2,
        4 * sources * rows * rest * columns,
        2 * sizes[-1] * inner * columns,
        24,
        [pltpu.VMEM((sources, rest, columns), BF16)],
    )(*hidden[-sources:], *downs[last:], *metas, shared, sums)

    gain = lax.dynamic_slice_in_dim(post_gain, tp[0] * columns, columns).reshape(1, columns)
    return call(
        functools.partial(final_kernel, width),
        shape((sources * rows, columns), BF16),
        [SMEM] + [VMEM] * (2 + sources),
        HBM,
        8 * sources * rows * columns,
        6 * sources * rows * columns,
        16,
        [pltpu.VMEM((sources * rows, columns), BF16), pltpu.SemaphoreType.DMA((sources,))],
    )(tp, combined, gain, *gather_all(squares, "tp", steps=False))


def plain(
    tokens, routes, gates, pre_gain, w_gate, w_up, w_down, sh_gate, sh_up, sh_down, post_gain, *, capacity
):
    tok_rows, full_width = tokens.shape
    experts_all = lax.axis_size("ep")
    inputs = tokens.astype(F32)
    scale_in = lax.rsqrt(jnp.mean(inputs * inputs, axis=1, keepdims=True) + EPS)
    normed = (inputs * scale_in * pre_gain[None, :]).astype(BF16)
    gate_shared = dot(normed, lax.all_gather(sh_gate, "tp", axis=0, tiled=True))
    up_shared = dot(normed, lax.all_gather(sh_up, "tp", axis=0, tiled=True))
    shared_hidden = (jax.nn.silu(gate_shared) * up_shared).astype(BF16)
    pair_count = tok_rows * TOPK
    expert_ids = routes.reshape(pair_count)
    matches = (expert_ids[:, None] == jnp.arange(experts_all, dtype=jnp.int32)[None, :]).astype(jnp.int32)
    earlier = jnp.cumsum(matches, axis=0) - matches
    dest_slot = expert_ids * capacity + jnp.sum(earlier * matches, axis=1)
    pair_token = jnp.arange(pair_count, dtype=jnp.int32) // TOPK
    slot_token = jnp.full((experts_all * capacity,), tok_rows, jnp.int32).at[dest_slot].set(pair_token)
    padded = jnp.concatenate([normed, jnp.zeros((1, full_width), BF16)], axis=0)
    outgoing = padded[slot_token].reshape(experts_all, capacity, full_width)
    arrived = lax.all_to_all(outgoing, "ep", split_axis=0, concat_axis=0, tiled=True)
    flat_rows = arrived.reshape(experts_all * capacity, full_width)
    hidden = (jax.nn.silu(dot(flat_rows, w_gate[0])) * dot(flat_rows, w_up[0])).astype(BF16)
    result = dot(hidden, w_down[0]).astype(BF16).reshape(arrived.shape)
    returned = lax.all_to_all(result, "ep", split_axis=0, concat_axis=0, tiled=True)
    picked = returned.reshape(experts_all * capacity, full_width)[dest_slot]
    weighted = picked.astype(F32) * gates.reshape(pair_count)[:, None]
    routed = jnp.sum(weighted.reshape(tok_rows, TOPK, full_width), axis=1).astype(BF16)
    shared = dot(shared_hidden, lax.all_gather(sh_down, "tp", axis=1, tiled=True)).astype(BF16)
    combined = routed.astype(F32) + shared.astype(F32)
    scale_out = lax.rsqrt(jnp.mean(combined * combined, axis=1, keepdims=True) + EPS)
    out_rows = (combined * scale_out * post_gain[None, :]).astype(BF16)
    return lax.all_to_all(out_rows, "tp", split_axis=1, concat_axis=0, tiled=True)


def folds(experts, sources):
    powers = experts & (experts - 1) == 0 and sources & (sources - 1) == 0
    return powers and experts >= 4 and sources >= 2


def per_device(tokens, *rest):
    experts, sources = lax.axis_size("ep"), lax.axis_size("tp")
    plan = folded if folds(experts, sources) else plain
    capacity = max(2, 4 * tokens.shape[0] * TOPK // (3 * experts))
    return plan(tokens, *rest, capacity=capacity)


def solution(mesh):
    return jax.shard_map(
        per_device,
        mesh=mesh,
        in_specs=(
            P(("ep", "tp"), None),
            P(("ep", "tp"), None),
            P(("ep", "tp"), None),
            P(),
            P("ep", None, None),
            P("ep", None, None),
            P("ep", None, None),
            P("tp", None),
            P("tp", None),
            P(None, "tp"),
            P(),
        ),
        out_specs=P("ep", "tp"),
        check_vma=False,
    )
```

```python
import functools

import jax
import jax.numpy as jnp
from jax import lax
from jax.experimental import pallas as pl
from jax.experimental.pallas import tpu as pltpu
from jax.sharding import PartitionSpec as P


TOPK = 2
LANES = 128
EPS = 1e-06
F32, BF16 = jnp.float32, jnp.bfloat16
VMEM = pl.BlockSpec(memory_space=pltpu.VMEM)
SMEM = pl.BlockSpec(memory_space=pltpu.SMEM)
HBM = pl.BlockSpec(memory_space=pltpu.HBM)


def dot(a, b):
    return jnp.dot(a, b, preferred_element_type=F32)


def silu(v):
    return v / (1.0 + jnp.exp(-v))


def pre_kernel(capacity, me_ref, tok_in, routes_in, gates_in, gain_in, normed_ref, meta_ref, *refs):
    *bufs, tok, routes_ref, gates_ref, gain_ref, held, arrival, sent = refs
    experts = len(bufs)
    fetches = [
        pltpu.make_async_copy(source, target, arrival.at[i])
        for i, (source, target) in enumerate(
            [(routes_in, routes_ref), (tok_in, tok), (gain_in, gain_ref), (gates_in, gates_ref)]
        )
    ]
    for fetch in fetches:
        fetch.start()
    rows = tok.shape[0]
    fetches[0].wait()
    padded = -(-experts // 16) * 16
    rel = jnp.bitwise_xor(routes_ref[...], me_ref[0])
    first, second = rel[0:1], rel[1:2]
    expert = lax.broadcasted_iota(jnp.int32, (padded, rows), 0)
    hit0, hit1 = (first == expert).astype(F32), (second == expert).astype(F32)
    above = (
        lax.broadcasted_iota(jnp.int32, (rows, rows), 0)
        < lax.broadcasted_iota(jnp.int32, (rows, rows), 1)
    ).astype(F32).astype(BF16)
    before0 = dot(hit0.astype(BF16), above)
    before1 = dot(hit1.astype(BF16), above) + jnp.sum(hit0, axis=1, keepdims=True)
    slot0 = jnp.sum(before0 * hit0, axis=0, keepdims=True).astype(jnp.int32)
    slot1 = jnp.sum(before1 * hit1, axis=0, keepdims=True).astype(jnp.int32)
    dest0, dest1 = first * capacity + slot0, second * capacity + slot1
    meta_ref[...] = jnp.zeros_like(meta_ref)
    meta_ref[0:1] = dest0.astype(F32)
    meta_ref[1:2] = dest1.astype(F32)
    for fetch in fetches[1:]:
        fetch.wait()
    meta_ref[2:4] = gates_ref[...]
    x = tok[...].astype(F32)
    scale = lax.rsqrt(jnp.mean(x * x, axis=1, keepdims=True) + EPS)
    normed = (x * scale * gain_ref[...]).astype(BF16)
    normed_ref[...] = normed
    copies = []
    half = experts // 2
    for group in (range(half, experts), range(half)):
        low = group[0] * capacity
        place = lax.broadcasted_iota(jnp.int32, (half * capacity, rows), 0) + low
        chosen = ((place == dest0) | (place == dest1)).astype(F32).astype(BF16)
        held[low : low + half * capacity] = dot(chosen, normed).astype(BF16)
        for j in group:
            copy = pltpu.make_async_copy(held.at[pl.ds(j * capacity, capacity)], bufs[j], sent.at[j])
            copy.start()
            copies.append(copy)
    for copy in copies:
        copy.wait()


def gated_kernel(*refs):
    parts, (gate_ref, up_ref), out_ref = refs[:-3], refs[-3:-1], refs[-1]
    rows = jnp.concatenate([part[...] for part in parts], axis=0)
    gate, up = dot(rows, gate_ref[0]), dot(rows, up_ref[0])
    out_ref[...] = (silu(gate) * up).astype(BF16)


def shared_kernel(count, tp_ref, normed_ref, *refs):
    gates, ups, out_ref = refs[:count], refs[count : 2 * count], refs[-1]
    depth = gates[0].shape[0]
    gate = up = None
    for m in range(count):
        at = pl.multiple_of(jnp.bitwise_xor(tp_ref[0], m) * depth, depth)
        part = normed_ref[:, pl.ds(at, depth)]
        g, u = dot(part, gates[m][...]), dot(part, ups[m][...])
        gate, up = (g, u) if m == 0 else (gate + g, up + u)
    out_ref[...] = (silu(gate) * up).astype(BF16)


def shared_out_kernel(*refs):
    parts, down_ref, out_ref = refs[:-2], refs[-2], refs[-1]
    rows = parts[0].shape[0]
    for m, part in enumerate(parts):
        out_ref[m * rows : (m + 1) * rows] = dot(part[...], down_ref[...]).astype(BF16)


def column(row, rows):
    return jnp.broadcast_to(row, (LANES, rows)).T[:, 0:1]


def choices(meta, first, slots):
    place = lax.broadcasted_iota(jnp.int32, (slots, meta.shape[1]), 0) + first
    return [
        (place == meta[k : k + 1].astype(jnp.int32)).astype(F32).astype(BF16) for k in range(TOPK)
    ]


def project(parts, pieces, result, at, capacity):
    rows, low = jnp.concatenate(parts, axis=0), 0
    for piece in pieces:
        out = dot(rows, piece[...]).astype(BF16)
        high = low + out.shape[1]
        for m in range(len(parts)):
            result[m, at : at + capacity, low:high] = out[m * capacity : (m + 1) * capacity]
        low = high


def weighted(chosen, meta, rows):
    total = None
    for k in range(TOPK):
        picked = lax.dot_general(chosen[k], rows, (((0,), (0,)), ((), ())), preferred_element_type=F32)
        term = picked * column(meta[TOPK + k : TOPK + k + 1], meta.shape[1])
        total = term if total is None else total + term
    return total


def project_all(hidden, downs, pieces, sizes, sources, result, capacity):
    j = used = 0
    for g, size in enumerate(sizes):
        for low in range(0, size * capacity, capacity):
            parts = [hidden[g * sources + m][low : low + capacity] for m in range(sources)]
            project(parts, downs[used : used + pieces[j]], result, j * capacity, capacity)
            used += pieces[j]
            j += 1


def early_kernel(sources, sizes, pieces, *refs, capacity):
    count = sources * len(sizes)
    hidden, downs = refs[:count], refs[count : count + sum(pieces)]
    metas, sums_ref, result = refs[count + sum(pieces) : -2], refs[-2], refs[-1]
    project_all(hidden, downs, pieces, sizes, sources, result, capacity)
    for m in range(sources):
        meta = metas[m][...]
        tokens = meta.shape[1]
        chosen = choices(meta, 0, result.shape[1])
        sums_ref[m * tokens : (m + 1) * tokens] = weighted(chosen, meta, result[m])


def late_kernel(sources, sizes, pieces, *refs, first, capacity):
    hidden, downs = refs[:sources], refs[sources : sources + sum(pieces)]
    metas, (shared_ref, sums_ref) = refs[sources + sum(pieces) : -5], refs[-5:-3]
    comb_ref, squares_ref, result = refs[-3:]
    project_all(hidden, downs, pieces, sizes, sources, result, capacity)
    for m in range(sources):
        meta = metas[m][...]
        tokens = meta.shape[1]
        here = slice(m * tokens, (m + 1) * tokens)
        chosen = choices(meta, first * capacity, result.shape[1])
        routed = sums_ref[here] + weighted(chosen, meta, result[m])
        combined = routed.astype(BF16).astype(F32) + shared_ref[here].astype(F32)
        comb_ref[here] = combined
        squares = jnp.sum(combined * combined, axis=1, keepdims=True)
        squares_ref[m : m + 1] = jnp.broadcast_to(squares, (tokens, LANES)).T[0:1]


def final_kernel(width, tp_ref, comb_ref, gain_ref, *refs):
    *squares, out_ref, held, sent = refs
    count = len(squares)
    tokens = comb_ref.shape[0] // count
    gain = gain_ref[...]
    copies = []
    for m in range(count):
        total = squares[0][m : m + 1]
        for d in range(1, count):
            total = total + squares[d][m ^ d : (m ^ d) + 1]
        scale = column(lax.rsqrt(total / width + EPS), tokens)
        here = slice(m * tokens, (m + 1) * tokens)
        held[here] = (comb_ref[here] * scale * gain).astype(BF16)
        at = pl.multiple_of(jnp.bitwise_xor(tp_ref[0], m) * tokens, 64)
        copy = pltpu.make_async_copy(
            held.at[pl.ds(m * tokens, tokens)], out_ref.at[pl.ds(at, tokens)], sent.at[m]
        )
        copy.start()
        copies.append(copy)
    for copy in copies:
        copy.wait()


def flip(value, axis, mask):
    size = lax.axis_size(axis)
    return lax.ppermute(value, axis, [(i, i ^ mask) for i in range(size)])


def spread(held, mask, axis):
    held = dict(held)
    while mask:
        for j in list(held):
            held[j ^ mask] = flip(held[j], axis, mask)
        mask //= 2
    return [held[j] for j in sorted(held)]


def two_routes(value, near):
    held, mask, last = {near: [value]}, near // 2, 2 * near - 1
    while mask:
        for j in list(held):
            place = j ^ mask
            if place == last and near > 2:
                half = value.shape[1] // 2
                other = held[last ^ (near // 2)][0][:, half:]
                held[place] = [flip(held[j][0][:, :half], "ep", mask), flip(other, "ep", near // 2)]
            else:
                held[place] = [flip(held[j][0], "ep", mask)]
        mask //= 2
    return [held[j] for j in sorted(held)]


def gather_all(value, axis, steps=True):
    size = lax.axis_size(axis)
    if steps:
        return spread({0: value}, size // 2, axis)
    return [value] + [flip(value, axis, j) for j in range(1, size)]


def shape(dims, kind):
    return jax.ShapeDtypeStruct(dims, kind)


def call(kernel, out_shape, in_specs, out_specs, flops, moved, limit, scratch_shapes=()):
    def run(*operands):
        return pl.pallas_call(
            kernel,
            out_shape=out_shape,
            in_specs=in_specs,
            out_specs=out_specs,
            scratch_shapes=scratch_shapes,
            compiler_params=pltpu.CompilerParams(vmem_limit_bytes=limit * 2**20),
            cost_estimate=pl.CostEstimate(
                flops=int(flops), bytes_accessed=int(moved), transcendentals=0
            ),
        )(*operands)

    return run


def expert_groups(experts):
    near, quarter = experts // 2, experts // 4
    return [range(near), range(near, near + quarter), range(near + quarter, experts)]


def folded(
    tokens, routes, gates, pre_gain, w_gate, w_up, w_down, sh_gate, sh_up, sh_down, post_gain, *, capacity
):
    rows, width = tokens.shape
    experts, sources = lax.axis_size("ep"), lax.axis_size("tp")
    inner, columns = w_down.shape[1], width // sources
    ep = lax.axis_index("ep").astype(jnp.int32).reshape(1)
    tp = lax.axis_index("tp").astype(jnp.int32).reshape(1)
    groups = expert_groups(experts)

    own_down = lax.dynamic_slice_in_dim(w_down[0], tp[0] * columns, columns, axis=1)
    near = experts // 2
    downs = [[down] for down in spread({0: own_down}, near // 2, "ep")]
    downs += two_routes(flip(own_down, "ep", near), near)

    normed, meta, *bufs = call(
        functools.partial(pre_kernel, capacity),
        [shape((rows, width), BF16), shape((8, rows), F32)] + [shape((capacity, width), BF16)] * experts,
        [SMEM] + [HBM] * 4,
        [VMEM, VMEM] + [HBM] * experts,
        2 * rows * experts * capacity * width,
        4 * rows * width,
        60,
        [
            pltpu.VMEM((rows, width), BF16),
            pltpu.VMEM((TOPK, rows), jnp.int32),
            pltpu.VMEM((TOPK, rows), F32),
            pltpu.VMEM((1, width), F32),
            pltpu.VMEM((experts * capacity, width), BF16),
            pltpu.SemaphoreType.DMA((4,)),
            pltpu.SemaphoreType.DMA((experts,)),
        ],
    )(ep, tokens, routes.T, gates.T, pre_gain.reshape(1, width))

    arrived = [bufs[0]] + [flip(bufs[j], "ep", j) for j in range(1, experts)]

    sh_gates, sh_ups = gather_all(sh_gate, "tp"), gather_all(sh_up, "tp")
    metas = gather_all(meta, "tp", steps=False)

    shared_hidden = call(
        functools.partial(shared_kernel, sources),
        shape((rows, sh_down.shape[0]), BF16),
        [SMEM] + [VMEM] * (1 + 2 * sources),
        VMEM,
        4 * rows * width * inner,
        4 * width * inner,
        16,
    )(tp, normed, *sh_gates, *sh_ups)
    shared = call(
        shared_out_kernel,
        shape((sources * rows, columns), BF16),
        [VMEM] * (sources + 1),
        VMEM,
        2 * sources * rows * inner * columns,
        2 * inner * columns,
        16,
    )(*gather_all(shared_hidden, "tp"), sh_down)

    hidden = []
    for blocks in groups:
        size = len(blocks)
        out = call(
            gated_kernel,
            shape((size * capacity, inner), BF16),
            [VMEM] * (size + 2),
            VMEM,
            4 * size * capacity * width * inner,
            4 * width * inner,
            16,
        )(*[arrived[j] for j in blocks], w_gate, w_up)
        back = []
        for b, j in enumerate(blocks):
            block = out[b * capacity : (b + 1) * capacity]
            back.append(block if j == 0 else flip(block, "ep", j))
        hidden += gather_all(jnp.concatenate(back, axis=0), "tp")

    sizes, last = [len(blocks) for blocks in groups], experts - len(groups[-1])
    sums_shape = shape((sources * rows, columns), F32)

    def flat(lists):
        return [item for items in lists for item in items]

    def summed(kernel, part, low, high, outs, *operands):
        return call(
            functools.partial(kernel, sources, part, [len(down) for down in downs[low:high]]),
            outs,
            [VMEM] * len(operands),
            [VMEM] * len(outs),
            4 * sources * rows * (high - low) * capacity * columns,
            2 * (high - low) * inner * columns,
            24,
            [pltpu.VMEM((sources, (high - low) * capacity, columns), BF16)],
        )(*operands)

    (sums,) = summed(
        functools.partial(early_kernel, capacity=capacity),
        sizes[:-1],
        0,
        last,
        [sums_shape],
        *hidden[:-sources],
        *flat(downs[:last]),
        *metas,
    )
    combined, squares = summed(
        functools.partial(late_kernel, first=last, capacity=capacity),
        sizes[-1:],
        last,
        experts,
        [sums_shape, shape((sources, rows), F32)],
        *hidden[-sources:],
        *flat(downs[last:]),
        *metas,
        shared,
        sums,
    )

    gain = lax.dynamic_slice_in_dim(post_gain, tp[0] * columns, columns).reshape(1, columns)
    return call(
        functools.partial(final_kernel, width),
        shape((sources * rows, columns), BF16),
        [SMEM] + [VMEM] * (2 + sources),
        HBM,
        8 * sources * rows * columns,
        6 * sources * rows * columns,
        16,
        [pltpu.VMEM((sources * rows, columns), BF16), pltpu.SemaphoreType.DMA((sources,))],
    )(tp, combined, gain, *gather_all(squares, "tp", steps=False))


def plain(
    tokens, routes, gates, pre_gain, w_gate, w_up, w_down, sh_gate, sh_up, sh_down, post_gain, *, capacity
):
    tok_rows, full_width = tokens.shape
    experts_all = lax.axis_size("ep")
    inputs = tokens.astype(F32)
    scale_in = lax.rsqrt(jnp.mean(inputs * inputs, axis=1, keepdims=True) + EPS)
    normed = (inputs * scale_in * pre_gain[None, :]).astype(BF16)
    gate_shared = dot(normed, lax.all_gather(sh_gate, "tp", axis=0, tiled=True))
    up_shared = dot(normed, lax.all_gather(sh_up, "tp", axis=0, tiled=True))
    shared_hidden = (jax.nn.silu(gate_shared) * up_shared).astype(BF16)
    pair_count = tok_rows * TOPK
    expert_ids = routes.reshape(pair_count)
    matches = (expert_ids[:, None] == jnp.arange(experts_all, dtype=jnp.int32)[None, :]).astype(jnp.int32)
    earlier = jnp.cumsum(matches, axis=0) - matches
    dest_slot = expert_ids * capacity + jnp.sum(earlier * matches, axis=1)
    pair_token = jnp.arange(pair_count, dtype=jnp.int32) // TOPK
    slot_token = jnp.full((experts_all * capacity,), tok_rows, jnp.int32).at[dest_slot].set(pair_token)
    padded = jnp.concatenate([normed, jnp.zeros((1, full_width), BF16)], axis=0)
    outgoing = padded[slot_token].reshape(experts_all, capacity, full_width)
    arrived = lax.all_to_all(outgoing, "ep", split_axis=0, concat_axis=0, tiled=True)
    flat_rows = arrived.reshape(experts_all * capacity, full_width)
    hidden = (jax.nn.silu(dot(flat_rows, w_gate[0])) * dot(flat_rows, w_up[0])).astype(BF16)
    result = dot(hidden, w_down[0]).astype(BF16).reshape(arrived.shape)
    returned = lax.all_to_all(result, "ep", split_axis=0, concat_axis=0, tiled=True)
    picked = returned.reshape(experts_all * capacity, full_width)[dest_slot]
    weighted = picked.astype(F32) * gates.reshape(pair_count)[:, None]
    routed = jnp.sum(weighted.reshape(tok_rows, TOPK, full_width), axis=1).astype(BF16)
    shared = dot(shared_hidden, lax.all_gather(sh_down, "tp", axis=1, tiled=True)).astype(BF16)
    combined = routed.astype(F32) + shared.astype(F32)
    scale_out = lax.rsqrt(jnp.mean(combined * combined, axis=1, keepdims=True) + EPS)
    out_rows = (combined * scale_out * post_gain[None, :]).astype(BF16)
    return lax.all_to_all(out_rows, "tp", split_axis=1, concat_axis=0, tiled=True)


def folds(experts, sources):
    powers = experts & (experts - 1) == 0 and sources & (sources - 1) == 0
    return powers and experts >= 4 and 2 <= sources <= 8


def per_device(tokens, *rest):
    experts, sources = lax.axis_size("ep"), lax.axis_size("tp")
    plan = folded if folds(experts, sources) else plain
    capacity = max(2, 4 * tokens.shape[0] * TOPK // (3 * experts))
    return plan(tokens, *rest, capacity=capacity)


def solution(mesh):
    return jax.shard_map(
        per_device,
        mesh=mesh,
        in_specs=(
            P(("ep", "tp"), None),
            P(("ep", "tp"), None),
            P(("ep", "tp"), None),
            P(),
            P("ep", None, None),
            P("ep", None, None),
            P("ep", None, None),
            P("tp", None),
            P("tp", None),
            P(None, "tp"),
            P(),
        ),
        out_specs=P("ep", "tp"),
        check_vma=False,
    )
```
